32 devices in a mesh: grp: 2 (over y), sp: 16 (over z, x, core), tp: 1.
Axes of the slice: x: 2, y: 2, z: 4, core: 2. Of those that a mesh axis runs over, the one named last changes fastest.
Arguments:
- tokens: bfloat16 [32768, 2048], P(('grp', 'sp')), parts along dimension 0, may hold values from -6 to 6
- doc_ids: int32 [32768], P(('grp', 'sp')), parts along dimension 0, may hold values from 0 to 3, never falling along the last dimension, each value on 1 to 8192 neighbouring positions
- gains: bfloat16 [2, 2048], replicated, may hold values from 0.099609375 to 1.8984375
- w_query: bfloat16 [2, 2048, 1024], P(None, None, 'tp'), may hold values from -0.125 to 0.125
- w_key: bfloat16 [2, 2048, 1024], P(None, None, 'tp'), may hold values from -0.125 to 0.125
- w_value: bfloat16 [2, 2048, 1024], P(None, None, 'tp'), may hold values from -0.125 to 0.125
- rel_table: float32 [2, 16, 257], P(None, 'tp'), may hold values from -6 to 270
- out_first: bfloat16 [1024, 2048], replicated, may hold values from -0.5 to 0.5
- out_last: bfloat16 [1024, 2048], P(None, 'tp'), may hold values from -0.5 to 0.5
Outputs:
- mixed: bfloat16 [32768, 2048], P(('grp', 'sp'), 'tp'), parts along dimension 0
The draws below stay inside these ranges and needn't reach their ends.
There are 2 independent parts, one for each index of `grp`. The reference program is written for one: setup_inputs(seed, part) draws one part's arguments, and reference() takes and returns one part's arrays. A program takes and returns all parts, laid end to end along the dimension named above; an argument that names none is the same for every part. Nothing has to cross between parts.
Inputs may be any that keep to these rules, and one draw needn't show every extreme that they name: `doc_ids`: document numbers never fall along the sequence.
All inputs are finite; a program needn't handle non-finite values.
Results may differ from the reference program's by a relative error of at most 0.014.
Values may be sent and summed in bfloat16 or wider, within the bound.
A program may use at most 320 MiB of HBM per device.

```python
import math
import jax
import jax.numpy as jnp
import numpy as np
from jax import lax

D = 2048
HEADS = 16
HEAD_DIM = 64
SEG = 64
PREV_SEGS = 8
MAX_REL = 128
LAYERS = 2
TOKENS = 16384
DOCS = 4


def draw_rel_table(key, part):
    shape = (LAYERS, HEADS, 2 * MAX_REL + 1)
    return jnp.clip(jax.random.normal(key, shape, jnp.float32), -4.0, 4.0)


def shard_levels(stream_key, dims, shards, smallest, largest):
    def one(position, parts):
        heights = jax.random.uniform(jax.random.fold_in(jax.random.fold_in(stream_key, 6), position), (parts,), jnp.float32, smallest / len(shards), largest / len(shards))
        return jnp.repeat(jnp.exp(heights), dims[position] // parts).reshape((-1,) + (1,) * (len(dims) - position - 1))

    factor_of = one(*shards[0])
    for cut in shards[1:]:
        factor_of = factor_of * one(*cut)
    return factor_of


def profile(count, total, limit, skew):
    weights = [(1 << 20) // math.isqrt(rank ** skew) + 1 for rank in range(2, count + 1)]
    surplus, counts = total - limit - (count - 1), [1] * (count - 1)
    while surplus > 0:
        movable = [i for i in range(count - 1) if counts[i] < limit]
        whole, remaining = sum([weights[i] for i in movable]), surplus
        for i in movable:
            addition = min(limit - counts[i], max(1, remaining * weights[i] // whole), surplus)
            counts[i] = counts[i] + addition
            surplus = surplus - addition
    return np.array([limit] + counts)


def ragged_sizes(stream_key, count, total, limit, lean):
    if count == 2:
        one = jax.random.randint(stream_key, (), max(1, total - limit), min(limit, total - 1) + 1)
        return jnp.stack([one, total - one])
    tallies = jnp.asarray(profile(count, total, limit, lean), jnp.int32)
    pairs = (count - 1) // 2
    source_of, taker = tallies[1:1 + 2 * pairs:2], tallies[2:2 + 2 * pairs:2]
    room = jnp.minimum(source_of - 1, limit - taker)
    passed = jax.random.randint(jax.random.fold_in(stream_key, 1), (pairs,), 0, 1 << 20) % (room + 1)
    tallies = tallies.at[1:1 + 2 * pairs:2].set(source_of - passed).at[2:2 + 2 * pairs:2].set(taker + passed)
    return tallies[jax.random.permutation(jax.random.fold_in(stream_key, 2), count)]


def gaussian(rng, shape, scale, most, pieces=(), kind=jnp.bfloat16):
    array = scale * jax.random.normal(rng, shape, jnp.float32)
    if pieces:
        array = array * shard_levels(rng, shape, pieces, -0.22, 0.18)
    return jnp.clip(array, -most, most).astype(kind)


def setup_inputs(seed: int = 0, part: int = 0) -> dict:
    splits = jax.random.split(jax.random.key(seed), 10)
    part_splits = jax.random.split(jax.random.fold_in(splits[9], part), 10)
    tokens = gaussian(part_splits[0], (TOKENS, D), 1.0, 6.0, ((0, 16),))
    doc_ids = jnp.searchsorted(jnp.cumsum(ragged_sizes(part_splits[1], DOCS, TOKENS, TOKENS // 2, 1)), jnp.arange(TOKENS), side="right").astype(jnp.int32)
    gains = jnp.clip(1.0 + 0.18 * jax.random.normal(splits[2], (LAYERS, D), jnp.float32), 0.099609375, 1.8984375).astype(jnp.bfloat16)
    w_query = gaussian(splits[3], (LAYERS, D, HEADS * HEAD_DIM), D ** -0.5, 0.125)
    w_key = gaussian(splits[4], (LAYERS, D, HEADS * HEAD_DIM), D ** -0.5, 0.125)
    w_value = gaussian(splits[5], (LAYERS, D, HEADS * HEAD_DIM), D ** -0.5, 0.125)
    rel_table = draw_rel_table(jax.random.fold_in(splits[9], 71), part)
    out_first = gaussian(splits[7], (HEADS * HEAD_DIM, D), (HEADS * HEAD_DIM // 9) ** -0.5, 0.5)
    out_last = gaussian(splits[8], (HEADS * HEAD_DIM, D), (HEADS * HEAD_DIM // 9) ** -0.5, 0.5)
    return {"tokens": tokens, "doc_ids": doc_ids, "gains": gains, "w_query": w_query, "w_key": w_key, "w_value": w_value, "rel_table": rel_table, "out_first": out_first, "out_last": out_last}


def normalize(stream, gain_row):
    values32 = stream.astype(jnp.float32)
    scaled = values32 * lax.rsqrt(lax.optimization_barrier(jnp.mean(values32 * values32, axis=-1, keepdims=True)) + 1e-06)
    return (scaled * gain_row.astype(jnp.float32)).astype(jnp.bfloat16)

def banded(key_rows, seg_count):
    by_segment = key_rows.reshape((seg_count + PREV_SEGS, SEG) + key_rows.shape[1:])
    stacked = jnp.stack([by_segment[offset_seg:offset_seg + seg_count] for offset_seg in range(PREV_SEGS + 1)], axis=1)
    return stacked.reshape((seg_count, (PREV_SEGS + 1) * SEG) + key_rows.shape[1:])

def attend(queries, pad_keys, pad_values, query_docs, pad_docs, bias_table):
    seq_rows = queries.shape[0]
    seg_count = seq_rows // SEG
    head_count = bias_table.shape[0]
    head_width = queries.shape[1] // head_count
    band_rows = (PREV_SEGS + 1) * SEG
    query_blocks = queries.reshape(seg_count, SEG, head_count, head_width).astype(jnp.float32)
    key_band = banded(pad_keys.reshape(-1, head_count, head_width), seg_count).astype(jnp.float32)
    value_band = banded(pad_values.reshape(-1, head_count, head_width), seg_count).astype(jnp.float32)
    query_pos = jnp.arange(SEG, dtype=jnp.int32)[:, None]
    band_pos = jnp.arange(band_rows, dtype=jnp.int32)[None, :]
    rel_index = jnp.clip(PREV_SEGS * SEG + query_pos - band_pos, -MAX_REL, MAX_REL) + MAX_REL
    bias = jnp.take(bias_table.astype(jnp.float32), rel_index, axis=1)
    scores = jnp.einsum('nqhd,nkhd->nhqk', query_blocks, key_band) * head_width ** (-0.5) + bias[None]
    doc_band = banded(pad_docs, seg_count)
    allowed = doc_band[:, None, None, :] == query_docs.reshape(seg_count, 1, SEG, 1)
    scores = jnp.where(allowed, scores, jnp.float32(-1e+30))
    row_max = lax.optimization_barrier(jnp.max(scores, axis=-1, keepdims=True))
    exp_scores = jnp.exp(scores - row_max)
    probs = exp_scores / lax.optimization_barrier(jnp.sum(exp_scores, axis=-1, keepdims=True))
    weights = probs.astype(jnp.bfloat16).astype(jnp.float32)
    result = jnp.einsum('nhqk,nkhd->nqhd', weights, value_band)
    return result.astype(jnp.bfloat16).reshape(seq_rows, head_count * head_width)

def reference(tokens, doc_ids, gains, w_query, w_key, w_value, rel_table, out_first, out_last):
    reach_rows = PREV_SEGS * SEG
    pad_docs = jnp.concatenate([jnp.full((reach_rows,), -1, jnp.int32), doc_ids.astype(jnp.int32)])
    hidden = tokens
    for layer_number in range(LAYERS):
        normed = normalize(hidden, gains[layer_number])
        queries = jnp.dot(normed, w_query[layer_number], preferred_element_type=jnp.float32).astype(jnp.bfloat16)
        keys = jnp.dot(normed, w_key[layer_number], preferred_element_type=jnp.float32).astype(jnp.bfloat16)
        values = jnp.dot(normed, w_value[layer_number], preferred_element_type=jnp.float32).astype(jnp.bfloat16)
        blank = jnp.zeros((reach_rows, keys.shape[1]), jnp.bfloat16)
        attended = attend(queries, jnp.concatenate([blank, keys]), jnp.concatenate([blank, values]), doc_ids, pad_docs, rel_table[layer_number])
        weight = out_first if layer_number == 0 else out_last
        update = jnp.dot(attended, weight, preferred_element_type=jnp.float32)
        hidden = (hidden.astype(jnp.float32) + update).astype(jnp.bfloat16)
    return hidden
```

```python
import functools

import jax
import jax.numpy as jnp
from jax import lax
from jax.experimental import pallas as pl
from jax.experimental.pallas import tpu as pltpu
from jax.sharding import PartitionSpec as P

SEG = 64
PREV_SEGS = 8
MAX_REL = 128
LAYERS = 2
DOCS = 4
REACH = SEG * PREV_SEGS
TILE = 128
LANES = 128
NEAR = 2 * MAX_REL
BAND = REACH + TILE
BLOCKED = -1e30
LOG2E = 1.4426950408889634


def from_behind(array, axis, by):
    size = lax.axis_size(axis)
    pairs = [(i, i + by) for i in range(size) if 0 <= i + by < size]
    return lax.ppermute(array, axis, pairs)


def normalize(stream, gain_row):
    values32 = stream.astype(jnp.float32)
    scaled = values32 * lax.rsqrt(jnp.mean(values32 * values32, axis=-1, keepdims=True) + 1e-06)
    return (scaled * gain_row.astype(jnp.float32)).astype(jnp.bfloat16)


def query_features(docs):
    rows = docs.shape[0]
    lane = jnp.arange(LANES, dtype=jnp.int32)[None, :]
    segment = (jnp.arange(rows, dtype=jnp.int32) // SEG % PREV_SEGS)[:, None]
    hit = (lane == docs[:, None]) | (lane == DOCS) | (lane == DOCS + 1 + segment)
    return hit.astype(jnp.bfloat16)


def key_features(docs, valid, first_segment):
    rows = docs.shape[0]
    lane = jnp.arange(LANES, dtype=jnp.int32)[None, :]
    segment = (jnp.arange(rows, dtype=jnp.int32) // SEG % PREV_SEGS + first_segment)[:, None]
    wanted = lane - (DOCS + 1)
    other_doc = (lane < DOCS) & (lane != docs[:, None])
    missing = (lane == DOCS) & ~valid[:, None]
    out_of_band = (wanted >= 0) & (wanted < PREV_SEGS)
    out_of_band &= (segment > wanted) | (segment < wanted - PREV_SEGS)
    return jnp.where(other_doc | missing | out_of_band, BLOCKED, 0.0).astype(jnp.bfloat16)


def bias_rows(table):
    heads = table.shape[0]
    shifted = (table - table[:, 2 * MAX_REL :]) * LOG2E
    flipped = jnp.flip(shifted, axis=1)[:, :NEAR]
    row = jnp.concatenate([flipped, jnp.zeros((heads, NEAR), jnp.float32)], axis=1)
    return row.reshape(heads // 2, 2, 2 * NEAR)


def attention_kernel(
    q_ref, kp_ref, kc_ref, vp_ref, vc_ref, qf_ref, kfp_ref, kfc_ref, u_ref, o_ref, k_s, v_s, t_s
):
    @pl.when(pl.program_id(1) == 0)
    def _():
        k_s[:REACH, LANES:] = kfp_ref[...]
        k_s[REACH:, LANES:] = kfc_ref[...]
        v_s[:, LANES:] = jnp.ones((2 * REACH, LANES), jnp.bfloat16)

    k_s[:REACH, :LANES] = kp_ref[...]
    k_s[REACH:, :LANES] = kc_ref[...]
    v_s[:REACH, :LANES] = vp_ref[...]
    v_s[REACH:, :LANES] = vc_ref[...]
    for head in range(2):
        wide = jnp.broadcast_to(u_ref[0, head : head + 1, :], (TILE, 2 * NEAR))
        rolled = pltpu.roll(wide, 0, 1, stride=1, stride_axis=0)
        t_s[head * TILE : (head + 1) * TILE, :] = rolled[:, :NEAR]
    first = lax.broadcasted_iota(jnp.int32, (TILE, LANES), 1) < LANES // 2
    for tile in range(REACH // TILE):
        rows = pl.ds(tile * TILE, TILE)
        band = pl.ds(tile * TILE, BAND)
        q = q_ref[rows, :]
        zero = jnp.zeros_like(q)
        feats = qf_ref[rows, :]
        pair = jnp.concatenate([jnp.where(first, q, zero), jnp.where(first, zero, q)], axis=0)
        wide_q = jnp.concatenate([pair, jnp.concatenate([feats, feats], axis=0)], axis=1)
        scores = lax.dot_general(
            wide_q, k_s[band, :], (((1,), (1,)), ((), ())), preferred_element_type=jnp.float32
        )
        far = scores[:, : BAND - NEAR]
        near = scores[:, BAND - NEAR :] + t_s[...]
        row_max = jnp.maximum(
            jnp.max(far, axis=1, keepdims=True), jnp.max(near, axis=1, keepdims=True)
        )
        weights = jnp.concatenate(
            [
                jnp.exp2(far - row_max).astype(jnp.bfloat16),
                jnp.exp2(near - row_max).astype(jnp.bfloat16),
            ],
            axis=1,
        )
        sums = jnp.dot(weights, v_s[band, :], preferred_element_type=jnp.float32)
        value = jnp.where(first, sums[:TILE, :LANES], sums[TILE:, :LANES])
        total = jnp.where(first, sums[:TILE, LANES:], sums[TILE:, LANES:])
        o_ref[rows, :] = (value / total).astype(o_ref.dtype)


def attend(q, k_prev, k_cur, v_prev, v_cur, qf, kf_prev, kf_cur, bias):
    rows, width = q.shape
    blocks, pairs = rows // REACH, width // LANES
    data = pl.BlockSpec((REACH, LANES), lambda b, p: (b, p))
    feature = pl.BlockSpec((REACH, LANES), lambda b, p: (b, 0))
    return pl.pallas_call(
        attention_kernel,
        grid=(blocks, pairs),
        in_specs=[data] * 5
        + [feature] * 3
        + [pl.BlockSpec((1, 2, 2 * NEAR), lambda b, p: (p, 0, 0))],
        out_specs=data,
        out_shape=jax.ShapeDtypeStruct((rows, width), jnp.bfloat16),
        scratch_shapes=[
            pltpu.VMEM((2 * REACH, 2 * LANES), jnp.bfloat16),
            pltpu.VMEM((2 * REACH, 2 * LANES), jnp.bfloat16),
            pltpu.VMEM((2 * TILE, NEAR), jnp.float32),
        ],
        compiler_params=pltpu.CompilerParams(dimension_semantics=("arbitrary", "arbitrary")),
        cost_estimate=pl.CostEstimate(
            flops=rows * pairs * 2 * BAND * 1024,
            bytes_accessed=rows * width * 12,
            transcendentals=rows * pairs * 2 * BAND,
        ),
        name="segment_attention",
    )(q, k_prev, k_cur, v_prev, v_cur, qf, kf_prev, kf_cur, bias)


def projected(normed, weight, factor=None):
    result = jnp.dot(normed, weight, preferred_element_type=jnp.float32)
    if factor is not None:
        result = result * jnp.float32(factor)
    return result.astype(jnp.bfloat16)


def shifted_back(low, high):
    return jnp.concatenate([low, high], axis=0)[: high.shape[0]]


def shards(tokens, doc_ids, gains, w_query, w_key, w_value, rel_table, out_first, out_last):
    row_count = tokens.shape[0]
    head_width = w_query.shape[2] // rel_table.shape[1]
    factor = LOG2E * head_width ** (-0.5)
    has_high = row_count > REACH
    far_docs = from_behind(doc_ids[row_count - REACH :], "sp", 1)
    is_first = lax.axis_index("sp") == 0
    far_valid = jnp.broadcast_to(~is_first, (REACH,))
    own_valid = jnp.ones((row_count,), jnp.bool_)
    qf = query_features(doc_ids)
    kf_far = key_features(far_docs, far_valid, -PREV_SEGS)
    kf_prev = key_features(doc_ids, own_valid, -PREV_SEGS)
    kf_cur = key_features(doc_ids, own_valid, 0)
    low, high = tokens[:REACH], tokens[REACH:]
    for layer in range(LAYERS):
        wq, wk, wv = w_query[layer], w_key[layer], w_value[layer]
        bias = bias_rows(rel_table[layer])
        weight = out_first if layer < LAYERS - 1 else out_last

        def residual(stream, attended):
            update = jnp.dot(
                lax.all_gather(attended, "tp", axis=1, tiled=True),
                weight,
                preferred_element_type=jnp.float32,
            )
            if layer == LAYERS - 1:
                cols = update.shape[1]
                stream = lax.dynamic_slice_in_dim(stream, lax.axis_index("tp") * cols, cols, 1)
            return (stream.astype(jnp.float32) + update).astype(jnp.bfloat16)

        if has_high:
            normed_high = normalize(high, gains[layer])
            k_high, v_high = projected(normed_high, wk), projected(normed_high, wv)
            far_k = from_behind(k_high[row_count - 2 * REACH :], "sp", 1)
            far_v = from_behind(v_high[row_count - 2 * REACH :], "sp", 1)
        normed_low = normalize(low, gains[layer])
        k_low, v_low = projected(normed_low, wk), projected(normed_low, wv)
        if has_high:
            q_high = projected(normed_high, wq, factor)
            attended = attend(
                q_high, shifted_back(k_low, k_high), k_high, shifted_back(v_low, v_high), v_high,
                qf[REACH:], kf_prev[: row_count - REACH], kf_cur[REACH:], bias,
            )
            next_high = residual(high, attended)
        else:
            far_k, far_v = from_behind(k_low, "sp", 1), from_behind(v_low, "sp", 1)
        q_low = projected(normed_low, wq, factor)
        attended = attend(
            q_low, far_k, k_low, far_v, v_low, qf[:REACH], kf_far, kf_cur[:REACH], bias
        )
        low = residual(low, attended)
        if has_high:
            high = next_high
    return jnp.concatenate([low, high], axis=0) if has_high else low


def solution(mesh):
    placed = (
        P(("grp", "sp"), None),
        P(("grp", "sp")),
        P(),
        P(None, None, "tp"),
        P(None, None, "tp"),
        P(None, None, "tp"),
        P(None, "tp", None),
        P(),
        P(None, "tp"),
    )
    return jax.shard_map(
        shards, mesh=mesh, in_specs=placed, out_specs=P(("grp", "sp"), "tp"), check_vma=False
    )
```

```python
import functools

import jax
import jax.numpy as jnp
from jax import lax
from jax.experimental import pallas as pl
from jax.experimental.pallas import tpu as pltpu
from jax.sharding import PartitionSpec as P

SEG = 64
PREV_SEGS = 8
MAX_REL = 128
LAYERS = 2
DOCS = 4
REACH = SEG * PREV_SEGS
TILE = 128
LANES = 128
NEAR = 2 * MAX_REL
BAND = REACH + TILE
BLOCKED = -1e30
COLS = 256
NORM_ROWS = 64
DOC_ROWS = 16
LOG2E = 1.4426950408889634


def from_behind(array, axis, by):
    size = lax.axis_size(axis)
    pairs = [(i, i + by) for i in range(size) if 0 <= i + by < size]
    return lax.ppermute(array, axis, pairs)


def query_features(docs):
    rows = docs.shape[0]
    lane = jnp.arange(LANES, dtype=jnp.int32)[None, :]
    segment = (jnp.arange(rows, dtype=jnp.int32) // SEG % PREV_SEGS)[:, None]
    hit = (lane == docs[:, None]) | (lane == DOCS) | (lane == DOCS + 1 + segment)
    return hit.astype(jnp.bfloat16)


def key_features(docs, valid, first_segment):
    rows = docs.shape[0]
    lane = jnp.arange(LANES, dtype=jnp.int32)[None, :]
    segment = (jnp.arange(rows, dtype=jnp.int32) // SEG % PREV_SEGS + first_segment)[:, None]
    wanted = lane - (DOCS + 1)
    other_doc = (lane < DOCS) & (lane != docs[:, None])
    missing = (lane == DOCS) & ~valid[:, None]
    out_of_band = (wanted >= 0) & (wanted < PREV_SEGS)
    out_of_band &= (segment > wanted) | (segment < wanted - PREV_SEGS)
    return jnp.where(other_doc | missing | out_of_band, BLOCKED, 0.0).astype(jnp.bfloat16)


def bias_rows(table):
    heads = table.shape[0]
    shifted = (table - table[:, 2 * MAX_REL :]) * LOG2E
    flipped = jnp.flip(shifted, axis=1)[:, :NEAR]
    row = jnp.concatenate([flipped, jnp.zeros((heads, NEAR), jnp.float32)], axis=1)
    return row.reshape(heads // 2, 2, 2 * NEAR)


def rms_scaled(values, gain):
    values32 = values.astype(jnp.float32)
    scale = lax.rsqrt(jnp.mean(values32 * values32, axis=-1, keepdims=True) + 1e-06)
    return (values32 * scale * gain.astype(jnp.float32)).astype(jnp.bfloat16)


def normalize_rows(source, gain, target, rows):
    @pl.loop(0, rows // NORM_ROWS)
    def _(step):
        at = pl.ds(pl.multiple_of(step * NORM_ROWS, NORM_ROWS), NORM_ROWS)
        target[at, :] = rms_scaled(source[at, :], gain)


def projection_kernel(factor, x_ref, g_ref, wq_ref, wk_ref, wv_ref, d_ref, q_ref, kv_ref, send_ref, n_s):
    rows = x_ref.shape[0]

    @pl.when(pl.program_id(0) == 0)
    def _():
        normalize_rows(x_ref, g_ref[...], n_s, rows)

    normed = n_s[...]
    for member, w_ref in ((0, wk_ref), (1, wv_ref)):
        piece = jnp.dot(normed, w_ref[0], preferred_element_type=jnp.float32).astype(jnp.bfloat16)
        kv_ref[member] = piece
        send_ref[member, :REACH] = piece[rows - REACH :]
        send_ref[member, REACH:] = d_ref[...]
    q = jnp.dot(normed, wq_ref[0], preferred_element_type=jnp.float32)
    q_ref[...] = (q * factor).astype(jnp.bfloat16)


def project_all(stream, gain, w_query, w_key, w_value, docs, layer, factor):
    rows, depth = stream.shape
    width = w_query.shape[2]
    cols = min(COLS, width)
    weight = pl.BlockSpec((1, depth, cols), lambda j: (layer, 0, j))
    return pl.pallas_call(
        functools.partial(projection_kernel, factor),
        grid=(width // cols,),
        in_specs=[
            pl.BlockSpec((rows, depth), lambda j: (0, 0)),
            pl.BlockSpec((1, depth), lambda j: (0, 0)),
            weight,
            weight,
            weight,
            pl.BlockSpec((DOC_ROWS, cols), lambda j: (0, 0)),
        ],
        out_specs=[
            pl.BlockSpec((rows, cols), lambda j: (0, j)),
            pl.BlockSpec((2, rows, cols), lambda j: (0, 0, j)),
            pl.BlockSpec((2, REACH + DOC_ROWS, cols), lambda j: (0, 0, j)),
        ],
        out_shape=[
            jax.ShapeDtypeStruct((rows, width), jnp.bfloat16),
            jax.ShapeDtypeStruct((2, rows, width), jnp.bfloat16),
            jax.ShapeDtypeStruct((2, REACH + DOC_ROWS, width), jnp.bfloat16),
        ],
        scratch_shapes=[pltpu.VMEM((rows, depth), jnp.bfloat16)],
        compiler_params=pltpu.CompilerParams(dimension_semantics=("arbitrary",)),
        cost_estimate=pl.CostEstimate(
            flops=rows * depth * width * 6,
            bytes_accessed=depth * width * 6 + rows * depth * 4,
            transcendentals=rows,
        ),
        name="project_all",
    )(stream, gain, w_query, w_key, w_value, docs)


def attend_pair(q_ref, qf_ref, u_ref, k_s, v_s, t_s, put):
    for head in range(2):
        wide = jnp.broadcast_to(u_ref[0, head : head + 1, :], (TILE, 2 * NEAR))
        rolled = pltpu.roll(wide, 0, 1, stride=1, stride_axis=0)
        t_s[head * TILE : (head + 1) * TILE, :] = rolled[:, :NEAR]
    first = lax.broadcasted_iota(jnp.int32, (TILE, LANES), 1) < LANES // 2
    for tile in range(REACH // TILE):
        rows = pl.ds(tile * TILE, TILE)
        band = pl.ds(tile * TILE, BAND)
        q = q_ref[rows, :]
        zero = jnp.zeros_like(q)
        feats = qf_ref[rows, :]
        pair = jnp.concatenate([jnp.where(first, q, zero), jnp.where(first, zero, q)], axis=0)
        wide_q = jnp.concatenate([pair, jnp.concatenate([feats, feats], axis=0)], axis=1)
        scores = lax.dot_general(
            wide_q, k_s[band, :], (((1,), (1,)), ((), ())), preferred_element_type=jnp.float32
        )
        far = scores[:, : BAND - NEAR]
        near = scores[:, BAND - NEAR :] + t_s[...]
        row_max = jnp.maximum(
            jnp.max(far, axis=1, keepdims=True), jnp.max(near, axis=1, keepdims=True)
        )
        weights = jnp.concatenate(
            [
                jnp.exp2(far - row_max).astype(jnp.bfloat16),
                jnp.exp2(near - row_max).astype(jnp.bfloat16),
            ],
            axis=1,
        )
        sums = jnp.dot(weights, v_s[band, :], preferred_element_type=jnp.float32)
        value = jnp.where(first, sums[:TILE, :LANES], sums[TILE:, :LANES])
        total = jnp.where(first, sums[:TILE, LANES:], sums[TILE:, LANES:])
        put(rows, (value / total).astype(jnp.bfloat16))


def layer_kernel(has_far, mixing, following, factor, layer, aliased, *refs):
    refs = list(refs)
    take = lambda n: [refs.pop(0) for _ in range(n)]
    q_ref, kc_ref, vc_ref, kp_ref, vp_ref, qf_ref, kfc_ref, kfp_ref, u_ref = take(9)
    if has_far:
        kx_ref, vx_ref, kfx_ref = take(3)
    if mixing:
        h_ref, wo_ref = take(2)
    if following:
        g_ref, d_ref, wq_ref, wk_ref, wv_ref = take(5)
    take(aliased)
    (o_ref,) = take(1)
    if following:
        qn_ref, kvn_ref, send_ref = take(3)
    k_s, v_s, t_s = take(3)
    block, pair = pl.program_id(0), pl.program_id(1)
    blocks, pairs = pl.num_programs(0), pl.num_programs(1)
    copies = []
    if mixing:
        a_s, wo_s, sems = take(3)
        copies.append(pltpu.make_async_copy(wo_ref, wo_s, sems.at[0]))
    if following:
        n_s, wq_s, wk_s, wv_s = take(4)
        for at, (source, target) in enumerate(((wk_ref, wk_s), (wv_ref, wv_s), (wq_ref, wq_s))):
            copies.append(pltpu.make_async_copy(source.at[layer + 1], target, sems.at[at + 1]))

    @pl.when((block == 0) & (pair == 0))
    def _():
        for copy in copies:
            copy.start()
        v_s[:, LANES:] = jnp.ones((2 * REACH, LANES), jnp.bfloat16)

    def fill(k_ref, v_ref, f_ref):
        k_s[:REACH, :LANES] = k_ref[0]
        v_s[:REACH, :LANES] = v_ref[0]
        k_s[:REACH, LANES:] = f_ref[...]

    if has_far:
        pl.when(block == 0)(lambda: fill(kx_ref, vx_ref, kfx_ref))
        pl.when(block > 0)(lambda: fill(kp_ref, vp_ref, kfp_ref))
    else:
        fill(kp_ref, vp_ref, kfp_ref)
    k_s[REACH:, :LANES] = kc_ref[0]
    k_s[REACH:, LANES:] = kfc_ref[...]
    v_s[REACH:, :LANES] = vc_ref[0]

    def put(rows, value):
        if mixing:
            a_s[pair, rows, :] = value
        else:
            o_ref[rows, :] = value

    attend_pair(q_ref, qf_ref, u_ref, k_s, v_s, t_s, put)
    if not mixing:
        return

    @pl.when(pair == pairs - 1)
    def _():
        @pl.when(block == 0)
        def _():
            copies[0].wait()

        attended = jnp.concatenate([a_s[i] for i in range(a_s.shape[0])], axis=1)
        depth = o_ref.shape[1]
        cols = min(COLS, depth)

        @pl.loop(0, depth // cols)
        def _(step):
            at = pl.ds(pl.multiple_of(step * cols, cols), cols)
            update = jnp.dot(attended, wo_s[:, at], preferred_element_type=jnp.float32)
            o_ref[:, at] = (h_ref[:, at].astype(jnp.float32) + update).astype(jnp.bfloat16)

        if following:
            @pl.when(block == 0)
            def _():
                for copy in copies[1:]:
                    copy.wait()

            normalize_rows(o_ref, g_ref[...], n_s, REACH)
            width = qn_ref.shape[1]
            wide = min(COLS, width)

            @pl.loop(0, width // wide)
            def _(step):
                at = pl.ds(pl.multiple_of(step * wide, wide), wide)
                normed = n_s[...]
                for member, w_s in ((0, wk_s), (1, wv_s)):
                    piece = jnp.dot(normed, w_s[:, at], preferred_element_type=jnp.float32)
                    piece = piece.astype(jnp.bfloat16)
                    kvn_ref[member, :, at] = piece
                    send_ref[member, :REACH, at] = piece
                    send_ref[member, REACH:, at] = d_ref[:, :wide]
                q = jnp.dot(normed, wq_s[:, at], preferred_element_type=jnp.float32)
                qn_ref[:, at] = (q * factor).astype(jnp.bfloat16)


def run_layer(
    q, kv, qf, kf_cur, kf_prev, bias, first_block, blocks, far=None, kf_far=None,
    stream=None, weight=None, following=None, held=(), layer=0, factor=1.0,
):
    rows, width = q.shape
    pairs = width // LANES
    mixing = weight is not None
    cur = lambda b: b + first_block
    prev = lambda b: jnp.maximum(b + first_block - 1, 0)
    member = lambda m, row: pl.BlockSpec((1, REACH, LANES), lambda b, p: (m, row(b), p))
    feature = lambda row: pl.BlockSpec((REACH, LANES), lambda b, p: (row(b), 0))
    zero = lambda b: 0
    anywhere = pl.BlockSpec(memory_space=pl.ANY)
    args = [q, kv, kv, kv, kv, qf, kf_cur, kf_prev, bias]
    specs = [
        pl.BlockSpec((REACH, LANES), lambda b, p: (cur(b), p)),
        member(0, cur), member(1, cur), member(0, prev), member(1, prev),
        feature(cur), feature(cur), feature(prev),
        pl.BlockSpec((1, 2, 2 * NEAR), lambda b, p: (p, 0, 0)),
    ]
    if far is not None:
        args += [far, far, kf_far]
        specs += [member(0, zero), member(1, zero), feature(zero)]
    scratch = [
        pltpu.VMEM((2 * REACH, 2 * LANES), jnp.bfloat16),
        pltpu.VMEM((2 * REACH, 2 * LANES), jnp.bfloat16),
        pltpu.VMEM((2 * TILE, NEAR), jnp.float32),
    ]
    if mixing:
        depth = stream.shape[1]
        whole_rows = pl.BlockSpec((REACH, depth), lambda b, p: (cur(b), 0))
        args += [stream, weight]
        specs += [whole_rows, anywhere]
        scratch += [
            pltpu.VMEM((pairs, REACH, LANES), jnp.bfloat16),
            pltpu.VMEM(weight.shape, jnp.bfloat16),
            pltpu.SemaphoreType.DMA((4,)),
        ]
        outs = [jax.ShapeDtypeStruct((rows, depth), jnp.bfloat16)]
        out_specs = [whole_rows]
    else:
        outs = [jax.ShapeDtypeStruct((rows, width), jnp.bfloat16)]
        out_specs = [pl.BlockSpec((REACH, LANES), lambda b, p: (cur(b), p))]
    flops = blocks * REACH * pairs * 2 * BAND * 1024
    if mixing:
        flops += blocks * REACH * width * depth * 2
    if following:
        flops += blocks * REACH * width * depth * 6
        gain, docs = following[:2]
        args += list(following)
        specs += [
            pl.BlockSpec(gain.shape, lambda b, p: (0, 0)),
            pl.BlockSpec(docs.shape, lambda b, p: (0, 0)),
        ] + [anywhere] * 3
        scratch += [pltpu.VMEM((REACH, depth), jnp.bfloat16)]
        scratch += [pltpu.VMEM((depth, width), jnp.bfloat16)] * 3
        outs += [
            jax.ShapeDtypeStruct((rows, width), jnp.bfloat16),
            jax.ShapeDtypeStruct((2, rows, width), jnp.bfloat16),
            jax.ShapeDtypeStruct((2, REACH + DOC_ROWS, width), jnp.bfloat16),
        ]
        out_specs += [
            pl.BlockSpec((REACH, width), lambda b, p: (cur(b), 0)),
            pl.BlockSpec((2, REACH, width), lambda b, p: (0, cur(b), 0)),
            pl.BlockSpec((2, REACH + DOC_ROWS, width), lambda b, p: (0, 0, 0)),
        ]
    aliases = {len(args) + at: at for at in range(len(held))}
    args += list(held)
    specs += [anywhere] * len(held)
    return pl.pallas_call(
        functools.partial(
            layer_kernel, far is not None, mixing, following is not None, factor, layer, len(held)
        ),
        grid=(blocks, pairs),
        in_specs=specs,
        out_specs=out_specs,
        out_shape=outs,
        scratch_shapes=scratch,
        input_output_aliases=aliases,
        compiler_params=pltpu.CompilerParams(dimension_semantics=("arbitrary", "arbitrary")),
        cost_estimate=pl.CostEstimate(
            flops=flops,
            bytes_accessed=blocks * REACH * width * 12,
            transcendentals=blocks * REACH * pairs * 2 * BAND,
        ),
        name="segment_layer",
    )(*args)


def shards(tokens, doc_ids, gains, w_query, w_key, w_value, rel_table, out_first, out_last):
    row_count = tokens.shape[0]
    width = w_query.shape[2]
    blocks = row_count // REACH
    factor = LOG2E * (width // rel_table.shape[1]) ** (-0.5)
    tail = doc_ids[row_count - REACH :].reshape(REACH // LANES, LANES) + 1
    docs = jnp.zeros((DOC_ROWS, min(COLS, width)), jnp.bfloat16)
    docs = docs.at[: REACH // LANES, :LANES].set(tail.astype(jnp.bfloat16))
    own_valid = jnp.ones((row_count,), jnp.bool_)
    qf = query_features(doc_ids)
    kf_prev = key_features(doc_ids, own_valid, -PREV_SEGS)
    kf_cur = key_features(doc_ids, own_valid, 0)
    bias = bias_rows(rel_table.reshape(-1, rel_table.shape[2]))
    bias = bias.reshape(LAYERS, -1, 2, 2 * NEAR)
    weights = (w_query, w_key, w_value)

    def far_features(far):
        marks = far[0, REACH : REACH + REACH // LANES, :LANES].astype(jnp.int32).reshape(REACH)
        return key_features(marks - 1, marks > 0, -PREV_SEGS)

    if lax.axis_size("tp") == 1 and blocks > 1 and LAYERS == 2:
        q, kv, sent = project_all(tokens, gains[:1], *weights, docs, 0, factor)
        far = from_behind(sent, "sp", 1)
        following = (gains[1:2], docs) + weights
        shared = dict(stream=tokens, weight=out_first, following=following, factor=factor)
        hidden, q_next, kv_next, sent = run_layer(
            q, kv, qf, kf_cur, kf_prev, bias[0], 1, blocks - 1, **shared
        )
        far_next = from_behind(sent, "sp", 1)
        kf_far = far_features(far)
        hidden, q_next, kv_next, _ = run_layer(
            q, kv, qf, kf_cur, kf_prev, bias[0], 0, 1, far=far, kf_far=kf_far,
            held=(hidden, q_next, kv_next), **shared
        )
        return run_layer(
            q_next, kv_next, qf, kf_cur, kf_prev, bias[1], 0, blocks, far=far_next,
            kf_far=kf_far, stream=hidden, weight=out_last,
        )[0]
    hidden = tokens
    for layer in range(LAYERS):
        q, kv, sent = project_all(hidden, gains[layer : layer + 1], *weights, docs, layer, factor)
        far = from_behind(sent, "sp", 1)
        attended = run_layer(
            q, kv, qf, kf_cur, kf_prev, bias[layer], 0, blocks, far=far, kf_far=far_features(far)
        )[0]
        weight = out_first if layer < LAYERS - 1 else out_last
        update = jnp.dot(
            lax.all_gather(attended, "tp", axis=1, tiled=True),
            weight,
            preferred_element_type=jnp.float32,
        )
        if layer == LAYERS - 1:
            cols = update.shape[1]
            hidden = lax.dynamic_slice_in_dim(hidden, lax.axis_index("tp") * cols, cols, 1)
        hidden = (hidden.astype(jnp.float32) + update).astype(jnp.bfloat16)
    return hidden


def solution(mesh):
    placed = (
        P(("grp", "sp"), None),
        P(("grp", "sp")),
        P(),
        P(None, None, "tp"),
        P(None, None, "tp"),
        P(None, None, "tp"),
        P(None, "tp", None),
        P(),
        P(None, "tp"),
    )
    return jax.shard_map(
        shards, mesh=mesh, in_specs=placed, out_specs=P(("grp", "sp"), "tp"), check_vma=False
    )
```
